32 devices in a mesh: sp: 8 (over z, y), dp: 4 (over x, core).
Axes of the slice: x: 2, y: 2, z: 4, core: 2. Of those that a mesh axis runs over, the one named last changes fastest.
Arguments:
- stream: bfloat16 [4, 1024, 2048], P('dp', 'sp'), may hold values from -6 to 6
- queries: bfloat16 [4, 1024, 1024], P('dp', 'sp'), may hold values from -6 to 6
- keys_in: bfloat16 [4, 1024, 1024], P('dp', 'sp'), may hold values from -6 to 6
- values_in: bfloat16 [4, 1024, 1024], P('dp', 'sp'), may hold values from -6 to 6
- key_shift: bfloat16 [4, 1024, 16], P('dp', 'sp'), may hold values from -8 to 16
- head_shift: float32 [16], replicated, may hold values from -16 to 0
- mix_gain: float32 [1024], replicated, may hold values from 0.1 to 1.9
- out_weight: bfloat16 [1024, 2048], replicated, may hold values from -0.1875 to 0.1875
- post_gain: float32 [2048], replicated, may hold values from 0.1 to 1.9
- route: int32 [4, 1024, 2], P('dp', 'sp'), may hold values from 0 to 31, as said below
- route_weight: float32 [4, 1024, 2], P('dp', 'sp'), may hold values from 0.25 to 1
- w_gate: bfloat16 [32, 2048, 1024], P(('sp', 'dp')), may hold values from -0.125 to 0.125
- w_up: bfloat16 [32, 2048, 1024], P(('sp', 'dp')), may hold values from -0.125 to 0.125
- w_down: bfloat16 [32, 1024, 2048], P(('sp', 'dp')), may hold values from -0.1875 to 0.1875
Outputs:
- result: bfloat16 [4, 1024, 2048], P('dp', 'sp')
The draws below stay inside these ranges and needn't reach their ends.
Inputs may be any that keep to these rules, and one draw needn't show every extreme that they name: `route`: each token names two different experts of one group (the group of expert e is e // 8). Of the 128 tokens of one device, each expert is named by at most 16; in every draw the 8 experts of one group are each named by exactly 16 tokens of every device.
All inputs are finite; a program needn't handle non-finite values.
Results may differ from the reference program's by a relative error of at most 0.0085.
Values may be sent and summed in bfloat16 or wider, within the bound.
A program may use at most 128 MiB of HBM per device.

```python
import math
import jax
import jax.numpy as jnp
from jax import lax

D = 2048
HEADS = 16
HD = 64
F = 1024
GROUPS = 4
TOK_DEV = 128
SEQUENCE_LENGTH = 1024
SEQUENCE_COUNT = 4
EXPERTS = 32
EPG = 8
CAP = 16
N_SP = 8
N_DP = 4


def head_rates(key):
    base = jax.random.fold_in(key, 11)
    share = jax.random.uniform(base, (HEADS,), jnp.float32, 0.4, 1.4)
    return -share * math.log(SEQUENCE_LENGTH)


def draw_head_shift(key, part):
    return head_rates(key)


def draw_key_shift(key, part):
    decay_rates = head_rates(key)
    random_jitter = jnp.clip(0.7 * jax.random.normal(jax.random.fold_in(key, 12), (SEQUENCE_COUNT, SEQUENCE_LENGTH // TOK_DEV, TOK_DEV, HEADS), jnp.float32), -3.0, 3.0)
    offset = jax.random.uniform(jax.random.fold_in(key, 13), (SEQUENCE_COUNT, SEQUENCE_LENGTH // TOK_DEV, 1, HEADS), jnp.float32, -0.7, 0.7)
    random_jitter = (random_jitter + offset).reshape(SEQUENCE_COUNT, SEQUENCE_LENGTH, HEADS)
    sudden_spike = jax.random.randint(jax.random.fold_in(key, 14), (SEQUENCE_COUNT, SEQUENCE_LENGTH, 1), 0, max(SEQUENCE_LENGTH // 4, 2)) == 0
    value_entry = jnp.where(sudden_spike, -decay_rates[None, None, :] - 0.7, random_jitter)
    return value_entry.astype(jnp.bfloat16)


def draw_route(key, part):
    nblocks = SEQUENCE_COUNT * (SEQUENCE_LENGTH // TOK_DEV)
    half = TOK_DEV // 2
    hot = jax.random.randint(jax.random.fold_in(key, 21), (), 0, GROUPS)
    cuts = jnp.sort(jax.random.randint(jax.random.fold_in(key, 22), (nblocks, GROUPS - 2), 0, half + 1), axis=1)
    bounds = jnp.concatenate([jnp.zeros((nblocks, 1), jnp.int32), cuts, jnp.full((nblocks, 1), half, jnp.int32)], axis=1)
    others = bounds[:, 1:] - bounds[:, :-1]
    sizes = jnp.concatenate([jnp.full((nblocks, 1), half, jnp.int32), others], axis=1)
    ends = jnp.cumsum(sizes, axis=1)
    starts = ends - sizes
    position = jnp.arange(TOK_DEV, dtype=jnp.int32)
    section = jnp.sum((position[None, :, None] >= ends[:, None, :]).astype(jnp.int32), axis=2)
    within = position[None, :] - jnp.take_along_axis(starts, section, axis=1)
    group = (hot + section) % GROUPS
    per_row = EPG // 2
    row_idx = within // per_row
    col_idx = within % per_row
    scores = jax.random.randint(jax.random.fold_in(key, 23), (nblocks, GROUPS, CAP, EPG), 0, 2 ** 20) * EPG + jnp.arange(EPG, dtype=jnp.int32)
    perm = jnp.argsort(scores, axis=-1, stable=True).astype(jnp.int32).reshape(nblocks, GROUPS * CAP * EPG)
    flat_idx = (section * CAP + row_idx) * EPG + 2 * col_idx
    first = jnp.take_along_axis(perm, flat_idx, axis=1) + group * EPG
    second = jnp.take_along_axis(perm, flat_idx + 1, axis=1) + group * EPG
    pairs = jnp.stack([first, second], axis=2)
    tscore = jax.random.randint(jax.random.fold_in(key, 24), (nblocks, TOK_DEV), 0, 2 ** 20) * TOK_DEV + position[None, :]
    placement = jnp.argsort(tscore, axis=1, stable=True).astype(jnp.int32)
    shuffled = jnp.take_along_axis(pairs, placement[:, :, None], axis=1)
    return shuffled.reshape(SEQUENCE_COUNT, SEQUENCE_LENGTH, 2).astype(jnp.int32)


def steps_of(rng, dims, cuts, low, high):
    loudness, own = 1.0, jax.random.fold_in(rng, 6)
    for axis_at, blocks in cuts:
        heights = jnp.exp(jax.random.uniform(jax.random.fold_in(own, axis_at), (blocks,), jnp.float32, low / len(cuts), high / len(cuts)))
        loudness = loudness * jnp.repeat(heights, dims[axis_at] // blocks).reshape([-1 if axis == axis_at else 1 for axis in range(len(dims))])
    return loudness


def noise(key, dims, scale, most, cuts=(), kind=jnp.bfloat16):
    drawn = scale * jax.random.normal(key, dims, jnp.float32)
    if cuts:
        drawn = drawn * steps_of(key, dims, cuts, -0.22, 0.18)
    return jnp.clip(drawn, -most, most).astype(kind)


def setup_inputs(seed: int = 0) -> dict:
    arg_keys = jax.random.split(jax.random.key(seed), 15)
    stream = noise(arg_keys[0], (SEQUENCE_COUNT, SEQUENCE_LENGTH, D), 1.0, 6.0, ((0, 4), (1, 8)))
    queries = noise(arg_keys[1], (SEQUENCE_COUNT, SEQUENCE_LENGTH, HEADS * HD), 1.0, 6.0, ((0, 4), (1, 8)))
    keys_in = noise(arg_keys[2], (SEQUENCE_COUNT, SEQUENCE_LENGTH, HEADS * HD), 1.0, 6.0, ((0, 4), (1, 8)))
    values_in = noise(arg_keys[3], (SEQUENCE_COUNT, SEQUENCE_LENGTH, HEADS * HD), 1.0, 6.0, ((0, 4), (1, 8)))
    key_shift = draw_key_shift(jax.random.fold_in(arg_keys[14], 71), 0)
    head_shift = draw_head_shift(jax.random.fold_in(arg_keys[14], 71), 0)
    mix_gain = jnp.clip(1.0 + 0.18 * jax.random.normal(arg_keys[6], (HEADS * HD,), jnp.float32), 0.1, 1.9)
    out_weight = noise(arg_keys[7], (HEADS * HD, D), (HEADS * HD) ** -0.5, 0.1875)
    post_gain = jnp.clip(1.0 + 0.18 * jax.random.normal(arg_keys[8], (D,), jnp.float32), 0.1, 1.9)
    route = draw_route(jax.random.fold_in(arg_keys[14], 71), 0)
    route_weight = jnp.clip(jnp.exp(math.log(1.0) - 1.3862944 * jax.random.uniform(arg_keys[10], (SEQUENCE_COUNT, SEQUENCE_LENGTH, 2), jnp.float32) ** steps_of(arg_keys[10], (SEQUENCE_COUNT, SEQUENCE_LENGTH, 2), ((0, 4), (1, 8)), -0.2, 0.2)), 0.25, 1.0)
    w_gate = noise(arg_keys[11], (EXPERTS, D, F), D ** -0.5, 0.125, ((0, 32),))
    w_up = noise(arg_keys[12], (EXPERTS, D, F), D ** -0.5, 0.125, ((0, 32),))
    w_down = noise(arg_keys[13], (EXPERTS, F, D), F ** -0.5, 0.1875, ((0, 32),))
    return dict(stream=stream, queries=queries, keys_in=keys_in, values_in=values_in, key_shift=key_shift, head_shift=head_shift, mix_gain=mix_gain, out_weight=out_weight, post_gain=post_gain, route=route, route_weight=route_weight, w_gate=w_gate, w_up=w_up, w_down=w_down)


norm_eps = 1e-05

def block_total(length):
    blocks = 1
    while blocks * 2 <= min(8, length // 512):
        blocks = blocks * 2
    return blocks

def stick_head(queries_head, keys_head, values_head, offsets):
    length = queries_head.shape[0]
    blocks = block_total(length)
    width = length // blocks
    scale = 1.0 / math.sqrt(HD)
    pieces = []
    for block_idx in range(blocks):
        begin = block_idx * width
        finish = begin + width
        logits = jnp.dot(queries_head[begin:finish].astype(jnp.float32), keys_head[:finish].astype(jnp.float32).T, precision=lax.Precision.HIGHEST, preferred_element_type=jnp.float32) * scale
        logits = logits + offsets[None, :finish]
        rows_pos = begin + jnp.arange(width, dtype=jnp.int32)
        cols_pos = jnp.arange(finish, dtype=jnp.int32)
        causal = cols_pos[None, :] < rows_pos[:, None]
        breaks = jnp.where(causal, jax.nn.log_sigmoid(-logits), 0.0)
        suffix = lax.cumsum(breaks, axis=1, reverse=True) - breaks
        weights = jnp.where(causal, jnp.exp(jax.nn.log_sigmoid(logits) + suffix), 0.0).astype(jnp.bfloat16)
        pieces.append(jnp.dot(weights.astype(jnp.float32), values_head[:finish].astype(jnp.float32), precision=lax.Precision.HIGHEST, preferred_element_type=jnp.float32))
    return jnp.concatenate(pieces, axis=0)

def reference(stream, queries, keys_in, values_in, key_shift, head_shift, mix_gain, out_weight, post_gain, route, route_weight, w_gate, w_up, w_down):

    def by_head(array):
        return array.reshape(SEQUENCE_COUNT, SEQUENCE_LENGTH, HEADS, HD).transpose(0, 2, 1, 3).reshape(SEQUENCE_COUNT * HEADS, SEQUENCE_LENGTH, HD)
    offsets = key_shift.astype(jnp.float32).transpose(0, 2, 1) + head_shift[None, :, None]
    offsets = offsets.reshape(SEQUENCE_COUNT * HEADS, SEQUENCE_LENGTH)

    def one_head(items):
        return stick_head(items[0], items[1], items[2], items[3]).astype(jnp.bfloat16)
    attended = lax.map(one_head, (by_head(queries), by_head(keys_in), by_head(values_in), offsets))
    attended = attended.reshape(SEQUENCE_COUNT, HEADS, SEQUENCE_LENGTH, HD).transpose(0, 2, 1, 3).reshape(SEQUENCE_COUNT * SEQUENCE_LENGTH, HEADS * HD)
    att32 = attended.astype(jnp.float32)
    normed = (att32 * lax.rsqrt(lax.optimization_barrier(jnp.mean(att32 * att32, axis=1, keepdims=True)) + norm_eps) * mix_gain).astype(jnp.bfloat16)
    mixed = jnp.dot(normed.astype(jnp.float32), out_weight.astype(jnp.float32), precision=lax.Precision.HIGHEST, preferred_element_type=jnp.float32)
    summed = stream.reshape(SEQUENCE_COUNT * SEQUENCE_LENGTH, D).astype(jnp.float32) + mixed
    hidden = (summed * lax.rsqrt(lax.optimization_barrier(jnp.mean(summed * summed, axis=1, keepdims=True)) + norm_eps) * post_gain).astype(jnp.bfloat16)
    total = SEQUENCE_COUNT * SEQUENCE_LENGTH
    expert_ids = route.reshape(total * 2).astype(jnp.int32)
    weights_flat = route_weight.reshape(total * 2)
    order = jnp.argsort(expert_ids, stable=True).astype(jnp.int32)
    tok_sorted = order // 2
    weight_sorted = weights_flat[order]
    counts = lax.optimization_barrier(jnp.sum((expert_ids[:, None] == jnp.arange(EXPERTS, dtype=jnp.int32)[None, :]).astype(jnp.int32), axis=0))
    starts = (jnp.cumsum(counts) - counts).astype(jnp.int32)
    most_rows = N_SP * N_DP * CAP
    tok_padded = jnp.concatenate([tok_sorted, jnp.zeros((most_rows,), jnp.int32)])
    weight_padded = jnp.concatenate([weight_sorted, jnp.zeros((most_rows,), jnp.float32)])

    def one_expert(carry, expert):
        index_rows = lax.dynamic_slice(tok_padded, (starts[expert],), (most_rows,))
        weight_rows = lax.dynamic_slice(weight_padded, (starts[expert],), (most_rows,))
        valid = jnp.arange(most_rows, dtype=jnp.int32) < counts[expert]
        rows = hidden[index_rows].astype(jnp.float32)
        gate = jnp.dot(rows, w_gate[expert].astype(jnp.float32), precision=lax.Precision.HIGHEST, preferred_element_type=jnp.float32)
        upper = jnp.dot(rows, w_up[expert].astype(jnp.float32), precision=lax.Precision.HIGHEST, preferred_element_type=jnp.float32)
        inner = (jax.nn.silu(gate) * upper).astype(jnp.bfloat16)
        output = jnp.dot(inner.astype(jnp.float32), w_down[expert].astype(jnp.float32), precision=lax.Precision.HIGHEST, preferred_element_type=jnp.float32).astype(jnp.bfloat16)
        scaled_values = jnp.where(valid[:, None], weight_rows[:, None] * output.astype(jnp.float32), 0.0)
        return (carry.at[index_rows].add(scaled_values), None)
    moe_sum, _ = lax.scan(one_expert, jnp.zeros((total, D), jnp.float32), jnp.arange(EXPERTS, dtype=jnp.int32))
    result = (hidden.astype(jnp.float32) + moe_sum).astype(jnp.bfloat16)
    return result.reshape(SEQUENCE_COUNT, SEQUENCE_LENGTH, D)
```

```python
import functools
import math

import jax
import jax.numpy as jnp
from jax import lax
from jax.experimental import pallas as pl
from jax.experimental.pallas import tpu as pltpu
from jax.sharding import PartitionSpec as P

HD = 64
GROUPS = 4
MESH = pl.DeviceIdType.MESH
F32 = jnp.float32
BF16 = jnp.bfloat16
VLIM = 56 * 1024 * 1024

norm_eps = 1e-05


def vmem(count):
    return [pl.BlockSpec(memory_space=pltpu.VMEM)] * count


def swap_kernel(n, count, *refs):
    ins, outs = refs[:count], refs[count : 2 * count]
    send_sem, recv_sem, own_sem = refs[2 * count :]
    me = lax.axis_index("sp")
    dp = lax.axis_index("dp")
    barrier = pltpu.get_barrier_semaphore()
    for d in range(1, n):
        pl.semaphore_signal(
            barrier, inc=1, device_id=(lax.rem(me + d, n), dp), device_id_type=MESH
        )
    own = [
        pltpu.make_async_copy(ins[a].at[me], outs[a].at[me], own_sem.at[a]) for a in range(count)
    ]
    for copy in own:
        copy.start()
    pl.semaphore_wait(barrier, n - 1)
    copies = []
    for d in range(1, n):
        peer = lax.rem(me + d, n)
        for a in range(count):
            copies.append(
                pltpu.make_async_remote_copy(
                    src_ref=ins[a].at[peer],
                    dst_ref=outs[a].at[me],
                    send_sem=send_sem.at[a, d],
                    recv_sem=recv_sem.at[a, d],
                    device_id=(peer, dp),
                    device_id_type=MESH,
                )
            )
            copies[-1].start()
    for copy in own + copies:
        copy.wait()


def swap(n, collective, *arrays):
    count = len(arrays)
    return pl.pallas_call(
        functools.partial(swap_kernel, n, count),
        out_shape=[jax.ShapeDtypeStruct(a.shape, a.dtype) for a in arrays],
        in_specs=vmem(count),
        out_specs=vmem(count),
        scratch_shapes=[
            pltpu.SemaphoreType.DMA((count, n)),
            pltpu.SemaphoreType.DMA((count, n)),
            pltpu.SemaphoreType.DMA((count,)),
        ],
        compiler_params=pltpu.CompilerParams(
            collective_id=collective, has_side_effects=True, vmem_limit_bytes=VLIM
        ),
        name=f"swap{collective}",
    )(*arrays)


def attention_kernel(heads, qkv_ref, shift_ref, out_ref):
    blocks, rows, _ = qkv_ref.shape
    cols = heads * HD
    scale = 1.0 / math.sqrt(HD)
    row = lax.broadcasted_iota(jnp.int32, (2 * rows, 2 * rows), 0)
    col = lax.broadcasted_iota(jnp.int32, (2 * rows, 2 * rows), 1)
    source = jnp.where(row >= rows, row - rows, row)
    summer = jnp.where((col >= rows) | (source > col), 1.0, 0.0).astype(BF16)
    causal = lax.broadcasted_iota(jnp.int32, (rows, rows), 1) < lax.broadcasted_iota(
        jnp.int32, (rows, rows), 0
    )

    def tile(i, j, h, carry, total, diagonal):
        q = qkv_ref[i, :, h * HD : (h + 1) * HD]
        k = qkv_ref[j, :, cols + h * HD : cols + (h + 1) * HD]
        v = qkv_ref[j, :, 2 * cols + h * HD : 2 * cols + (h + 1) * HD]
        z = lax.dot_general(q, k, (((1,), (1,)), ((), ())), preferred_element_type=F32) * scale
        z = z + shift_ref[j, h : h + 1, :]
        soft = jnp.log(1.0 + jnp.exp(-jnp.abs(z)))
        breaks = -jnp.maximum(z, 0.0) - soft
        own = jnp.minimum(z, 0.0) - soft
        if diagonal:
            breaks = jnp.where(causal, breaks, 0.0)
        high = breaks.astype(BF16)
        low = (breaks - high.astype(F32)).astype(BF16)
        sums = jnp.dot(
            jnp.concatenate([high, low], axis=1), summer, preferred_element_type=F32
        )
        weight = jnp.exp(own + (sums[:, :rows] + carry))
        if diagonal:
            weight = jnp.where(causal, weight, 0.0)
        total = total + jnp.dot(weight.astype(BF16), v, preferred_element_type=F32)
        return carry + sums[:, rows:], total

    zero_carry = jnp.zeros((rows, rows), F32)
    zero_total = jnp.zeros((rows, HD), F32)

    for i in range(blocks):
        state = []
        for h in range(heads):
            state.extend(tile(i, i, h, zero_carry, zero_total, True))
        for j in range(i - 1, -1, -1):
            new = []
            for h in range(heads):
                new.extend(tile(i, j, h, state[2 * h], state[2 * h + 1], False))
            state = new
        out_ref[i] = jnp.concatenate([state[2 * h + 1] for h in range(heads)], axis=1).astype(BF16)


def attention(heads, qkv, shift):
    blocks, rows, _ = qkv.shape
    return pl.pallas_call(
        functools.partial(attention_kernel, heads),
        out_shape=jax.ShapeDtypeStruct((blocks, rows, heads * HD), BF16),
        in_specs=vmem(2),
        out_specs=vmem(1)[0],
        compiler_params=pltpu.CompilerParams(vmem_limit_bytes=VLIM),
        name="attention",
    )(qkv, shift)


def place(n_sp, n_dp):
    ny = n_sp // GROUPS
    sp, dp = lax.axis_index("sp"), lax.axis_index("dp")
    plane, y = sp // ny, lax.rem(sp, ny)
    member = y * n_dp + dp

    def at(g, m):
        return (g * ny + m // n_dp, lax.rem(m, n_dp))

    return plane, member, at


def greet(plane, member, at, per_group):
    barrier = pltpu.get_barrier_semaphore()
    for d in range(1, GROUPS):
        pl.semaphore_signal(
            barrier, inc=1, device_id=at(lax.rem(plane + d, GROUPS), member), device_id_type=MESH
        )
    for d in range(1, per_group):
        pl.semaphore_signal(
            barrier, inc=1, device_id=at(plane, lax.rem(member + d, per_group)), device_id_type=MESH
        )
    pl.semaphore_wait(barrier, GROUPS + per_group - 2)


def one_hot_rows(meta, row):
    lanes = lax.broadcasted_iota(jnp.int32, (meta.shape[1], meta.shape[1]), 0).astype(F32)
    return lanes == meta[row : row + 1, :]


def dispatch_kernel(
    n_sp,
    n_dp,
    packed,
    meta,
    got,
    got_meta,
    block,
    stage,
    z_send,
    z_recv,
    t_send,
    t_recv,
    p_send,
    p_recv,
    own_sem,
):
    _, per_group, cap, width = got.shape
    slots = packed.shape[1]
    chunk = min(512, width)
    plane, member, at = place(n_sp, n_dp)
    greet(plane, member, at, per_group)
    z_copies, t_copies = [None], [None]
    for d in range(1, GROUPS):
        other = lax.rem(plane + d, GROUPS)
        for kept, src, dst, send, recv in (
            (t_copies, meta, got_meta, t_send, t_recv),
            (z_copies, packed, block, z_send, z_recv),
        ):
            kept.append(
                pltpu.make_async_remote_copy(
                    src_ref=src.at[other],
                    dst_ref=dst.at[plane],
                    send_sem=send.at[d],
                    recv_sem=recv.at[d],
                    device_id=at(other, member),
                    device_id_type=MESH,
                )
            )
            kept[-1].start()
    got_meta[plane] = meta[plane]
    later = []
    for d in range(GROUPS):
        source = lax.rem(plane - d + GROUPS, GROUPS)
        if d:
            t_copies[d].wait_recv()
            z_copies[d].wait_recv()
        held = block if d else packed
        info = got_meta[source]
        hot = jnp.where(one_hot_rows(info, 0) | one_hot_rows(info, 1), 1.0, 0.0).astype(BF16)
        hot = hot[:, :slots]
        for c in range(0, width, chunk):
            rows = jnp.dot(hot, held[source, :, c : c + chunk], preferred_element_type=F32)
            for m in range(per_group):
                stage[source, m, :, c : c + chunk] = rows[m * cap : (m + 1) * cap].astype(BF16)
        own = pltpu.make_async_copy(stage.at[source, member], got.at[source, member], own_sem.at[d])
        own.start()
        later.append(own)
        for e in range(1, per_group):
            other = lax.rem(member + e, per_group)
            copy = pltpu.make_async_remote_copy(
                src_ref=stage.at[source, other],
                dst_ref=got.at[source, member],
                send_sem=p_send.at[d, e],
                recv_sem=p_recv.at[d, e],
                device_id=at(plane, other),
                device_id_type=MESH,
            )
            copy.start()
            later.append(copy)
    for copy in later:
        copy.wait()
    for d in range(1, GROUPS):
        t_copies[d].wait_send()
        z_copies[d].wait_send()


def dispatch(n_sp, n_dp, cap, packed, meta):
    per_group = n_sp * n_dp // GROUPS
    _, slots, width = packed.shape
    buffer = (GROUPS, per_group, cap, width)
    dma = pltpu.SemaphoreType.DMA
    return pl.pallas_call(
        functools.partial(dispatch_kernel, n_sp, n_dp),
        out_shape=[
            jax.ShapeDtypeStruct(buffer, BF16),
            jax.ShapeDtypeStruct(meta.shape, F32),
        ],
        in_specs=vmem(2),
        out_specs=vmem(2),
        scratch_shapes=[
            pltpu.VMEM(packed.shape, BF16),
            pltpu.VMEM(buffer, BF16),
            dma((GROUPS,)),
            dma((GROUPS,)),
            dma((GROUPS,)),
            dma((GROUPS,)),
            dma((GROUPS, per_group)),
            dma((GROUPS, per_group)),
            dma((GROUPS,)),
        ],
        compiler_params=pltpu.CompilerParams(
            collective_id=2, has_side_effects=True, vmem_limit_bytes=VLIM
        ),
        name="dispatch",
    )(packed, meta)


def combine_kernel(
    n_sp,
    n_dp,
    reply,
    meta,
    out,
    block,
    stage,
    z_send,
    z_recv,
    p_send,
    p_recv,
    own_sem,
):
    _, per_group, cap, width = reply.shape
    slots = out.shape[1]
    chunk = min(512, width)
    plane, member, at = place(n_sp, n_dp)
    greet(plane, member, at, per_group)
    order = list(range(1, GROUPS)) + [0]
    plane_copies = {}
    for d in order:
        target = lax.rem(plane + d, GROUPS)
        own = pltpu.make_async_copy(reply.at[target, member], block.at[target, member], own_sem.at[d])
        own.start()
        copies = [own]
        for e in range(1, per_group):
            other = lax.rem(member + e, per_group)
            copies.append(
                pltpu.make_async_remote_copy(
                    src_ref=reply.at[target, other],
                    dst_ref=block.at[target, member],
                    send_sem=p_send.at[d, e],
                    recv_sem=p_recv.at[d, e],
                    device_id=at(plane, other),
                    device_id_type=MESH,
                )
            )
            copies[-1].start()
        plane_copies[d] = copies
    z_copies = []
    for d in order:
        target = lax.rem(plane + d, GROUPS)
        for copy in plane_copies[d]:
            copy.wait()
        info = meta[target]
        spread = jnp.where(one_hot_rows(info, 0), info[2:3, :], 0.0) + jnp.where(
            one_hot_rows(info, 1), info[3:4, :], 0.0
        )
        spread = spread.T[:slots]
        high = spread.astype(BF16)
        low = (spread - high.astype(F32)).astype(BF16)
        for c in range(0, width, chunk):
            if cap % 16 == 0:
                rows = block[target, :, :, c : c + chunk].reshape(per_group * cap, chunk)
            else:
                rows = jnp.concatenate(
                    [block[target, m, :, c : c + chunk].astype(F32) for m in range(per_group)], axis=0
                ).astype(BF16)
            total = jnp.dot(high, rows, preferred_element_type=F32) + jnp.dot(
                low, rows, preferred_element_type=F32
            )
            if d:
                stage[target, :, c : c + chunk] = total.astype(BF16)
            else:
                out[target, :, c : c + chunk] = total.astype(BF16)
        if d:
            copy = pltpu.make_async_remote_copy(
                src_ref=stage.at[target],
                dst_ref=out.at[plane],
                send_sem=z_send.at[d],
                recv_sem=z_recv.at[d],
                device_id=at(target, member),
                device_id_type=MESH,
            )
            copy.start()
            z_copies.append(copy)
    for copy in z_copies:
        copy.wait()


def combine(n_sp, n_dp, slots, reply, meta):
    _, per_group, cap, width = reply.shape
    dma = pltpu.SemaphoreType.DMA
    return pl.pallas_call(
        functools.partial(combine_kernel, n_sp, n_dp),
        out_shape=jax.ShapeDtypeStruct((GROUPS, slots, width), BF16),
        in_specs=vmem(2),
        out_specs=vmem(1)[0],
        scratch_shapes=[
            pltpu.VMEM(reply.shape, BF16),
            pltpu.VMEM((GROUPS, slots, width), BF16),
            dma((GROUPS,)),
            dma((GROUPS,)),
            dma((GROUPS, per_group)),
            dma((GROUPS, per_group)),
            dma((GROUPS,)),
        ],
        compiler_params=pltpu.CompilerParams(
            collective_id=3, has_side_effects=True, vmem_limit_bytes=VLIM
        ),
        name="combine",
    )(reply, meta)


def on_device(
    n_sp,
    n_dp,
    stream,
    queries,
    keys_in,
    values_in,
    key_shift,
    head_shift,
    mix_gain,
    out_weight,
    post_gain,
    route,
    route_weight,
    w_gate,
    w_up,
    w_down,
):
    tokens, width = stream.shape[1], stream.shape[2]
    heads = key_shift.shape[2] // n_sp
    cols = heads * HD

    n_expert = n_sp * n_dp
    per_group = n_expert // GROUPS
    cap = tokens // per_group
    slots = tokens // 2
    expert_ids = route[0].reshape(tokens * 2)
    onehot = (expert_ids[:, None] == jnp.arange(n_expert, dtype=jnp.int32)[None, :]).astype(BF16)
    before = jnp.arange(tokens * 2)
    earlier = (before[:, None] > before[None, :]).astype(BF16)
    counts = jnp.dot(earlier, onehot, preferred_element_type=F32)
    ranks = jnp.sum(counts * onehot.astype(F32), axis=1)
    inside = lax.rem(expert_ids, per_group).astype(F32) * cap + ranks
    inside = inside.reshape(tokens, 2)
    token_group = route[0][:, 0] // per_group
    group_hot = (token_group[:, None] == jnp.arange(GROUPS, dtype=jnp.int32)[None, :]).astype(BF16)
    group_rank = jnp.sum(
        jnp.dot(earlier[:tokens, :tokens], group_hot, preferred_element_type=F32)
        * group_hot.astype(F32),
        axis=1,
    )
    slot = token_group * slots + group_rank.astype(jnp.int32)
    slot_hot = slot[None, :] == jnp.arange(GROUPS * slots, dtype=jnp.int32)[:, None]
    facts = jnp.concatenate([inside + 1.0, route_weight[0]], axis=1)
    table = jnp.sum(jnp.where(slot_hot[:, None, :], facts.T[None, :, :], 0.0), axis=2)
    table = table - jnp.array([1.0, 1.0, 0.0, 0.0], F32)[None, :]
    table = table.reshape(GROUPS, slots, 4).transpose(0, 2, 1)
    lanes = per_group * cap
    meta = jnp.full((GROUPS, 8, lanes), -1.0, F32).at[:, :4, :slots].set(table)

    def by_peer(array):
        return array[0].reshape(tokens, n_sp, cols).transpose(1, 0, 2)

    qkv = jnp.concatenate([by_peer(queries), by_peer(keys_in), by_peer(values_in)], axis=2)
    offsets = (key_shift[0].astype(F32) + head_shift[None, :]).T.reshape(n_sp, heads, tokens)
    offsets = jnp.pad(offsets, ((0, 0), (0, 8 - heads), (0, 0)))
    qkv, offsets = swap(n_sp, 0, qkv, offsets)
    attended = attention(heads, qkv, offsets)
    (attended,) = swap(n_sp, 1, attended)
    att32 = attended.transpose(1, 0, 2).reshape(tokens, n_sp * cols).astype(F32)
    normed = (
        att32 * lax.rsqrt(jnp.mean(att32 * att32, axis=1, keepdims=True) + norm_eps) * mix_gain
    ).astype(BF16)
    mixed = jnp.dot(normed, out_weight, preferred_element_type=F32)
    summed = stream[0].astype(F32) + mixed
    hidden = (
        summed * lax.rsqrt(jnp.mean(summed * summed, axis=1, keepdims=True) + norm_eps) * post_gain
    ).astype(BF16)

    slot_hot = slot_hot.astype(BF16)
    packed = jnp.dot(slot_hot, hidden, preferred_element_type=F32).astype(BF16)
    received, tables = dispatch(n_sp, n_dp, cap, packed.reshape(GROUPS, slots, width), meta)
    rows = received.reshape(GROUPS * per_group * cap, width)
    gate = jnp.dot(rows, w_gate[0], preferred_element_type=F32)
    upper = jnp.dot(rows, w_up[0], preferred_element_type=F32)
    inner = (jax.nn.silu(gate) * upper).astype(BF16)
    reply = jnp.dot(inner, w_down[0], preferred_element_type=F32).astype(BF16)
    returned = combine(n_sp, n_dp, slots, reply.reshape(received.shape), tables)
    moe_sum = lax.dot_general(
        slot_hot,
        returned.reshape(GROUPS * slots, width),
        (((0,), (0,)), ((), ())),
        preferred_element_type=F32,
    )
    return (hidden.astype(F32) + moe_sum).astype(BF16)[None]


def solution(mesh):
    return jax.shard_map(
        functools.partial(on_device, mesh.shape["sp"], mesh.shape["dp"]),
        mesh=mesh,
        in_specs=(
            P("dp", "sp", None),
            P("dp", "sp", None),
            P("dp", "sp", None),
            P("dp", "sp", None),
            P("dp", "sp", None),
            P(),
            P(),
            P(),
            P(),
            P("dp", "sp", None),
            P("dp", "sp", None),
            P(("sp", "dp"), None, None),
            P(("sp", "dp"), None, None),
            P(("sp", "dp"), None, None),
        ),
        out_specs=P("dp", "sp", None),
        check_vma=False,
    )
```

```python
import functools
import math

import jax
import jax.numpy as jnp
from jax import lax
from jax.experimental import pallas as pl
from jax.experimental.pallas import tpu as pltpu
from jax.sharding import PartitionSpec as P

HD = 64
GROUPS = 4
MESH = pl.DeviceIdType.MESH
F32 = jnp.float32
BF16 = jnp.bfloat16
VLIM = 56 * 1024 * 1024

norm_eps = 1e-05


def vmem(count):
    return [pl.BlockSpec(memory_space=pltpu.VMEM)] * count


def swap_kernel(n, count, *refs):
    ins, outs = refs[:count], refs[count : 2 * count]
    send_sem, recv_sem, own_sem = refs[2 * count :]
    me = lax.axis_index("sp")
    dp = lax.axis_index("dp")
    barrier = pltpu.get_barrier_semaphore()
    for d in range(1, n):
        pl.semaphore_signal(
            barrier, inc=1, device_id=(lax.rem(me + d, n), dp), device_id_type=MESH
        )
    own = [
        pltpu.make_async_copy(ins[a].at[me], outs[a].at[me], own_sem.at[a]) for a in range(count)
    ]
    for copy in own:
        copy.start()
    pl.semaphore_wait(barrier, n - 1)
    copies = []
    for d in range(1, n):
        peer = lax.rem(me + d, n)
        for a in range(count):
            copies.append(
                pltpu.make_async_remote_copy(
                    src_ref=ins[a].at[peer],
                    dst_ref=outs[a].at[me],
                    send_sem=send_sem.at[a, d],
                    recv_sem=recv_sem.at[a, d],
                    device_id=(peer, dp),
                    device_id_type=MESH,
                )
            )
            copies[-1].start()
    for copy in own + copies:
        copy.wait()


def swap(n, collective, *arrays):
    count = len(arrays)
    return pl.pallas_call(
        functools.partial(swap_kernel, n, count),
        out_shape=[jax.ShapeDtypeStruct(a.shape, a.dtype) for a in arrays],
        in_specs=vmem(count),
        out_specs=vmem(count),
        scratch_shapes=[
            pltpu.SemaphoreType.DMA((count, n)),
            pltpu.SemaphoreType.DMA((count, n)),
            pltpu.SemaphoreType.DMA((count,)),
        ],
        compiler_params=pltpu.CompilerParams(
            collective_id=collective, has_side_effects=True, vmem_limit_bytes=VLIM
        ),
        name=f"swap{collective}",
    )(*arrays)


def attention_kernel(heads, qkv_ref, shift_ref, out_ref):
    blocks, rows, _ = qkv_ref.shape
    cols = heads * HD
    scale = 1.0 / math.sqrt(HD)
    row = lax.broadcasted_iota(jnp.int32, (2 * rows, 2 * rows), 0)
    col = lax.broadcasted_iota(jnp.int32, (2 * rows, 2 * rows), 1)
    source = jnp.where(row >= rows, row - rows, row)
    summer = jnp.where((col >= rows) | (source > col), 1.0, 0.0).astype(BF16)
    causal = lax.broadcasted_iota(jnp.int32, (rows, rows), 1) < lax.broadcasted_iota(
        jnp.int32, (rows, rows), 0
    )

    def tile(i, j, h, carry, total, diagonal):
        q = qkv_ref[i, :, h * HD : (h + 1) * HD]
        k = qkv_ref[j, :, cols + h * HD : cols + (h + 1) * HD]
        v = qkv_ref[j, :, 2 * cols + h * HD : 2 * cols + (h + 1) * HD]
        z = lax.dot_general(q, k, (((1,), (1,)), ((), ())), preferred_element_type=F32) * scale
        z = z + shift_ref[j, h : h + 1, :]
        soft = jnp.log(1.0 + jnp.exp(-jnp.abs(z)))
        breaks = -jnp.maximum(z, 0.0) - soft
        own = jnp.minimum(z, 0.0) - soft
        if diagonal:
            breaks = jnp.where(causal, breaks, 0.0)
        high = breaks.astype(BF16)
        low = (breaks - high.astype(F32)).astype(BF16)
        sums = jnp.dot(
            jnp.concatenate([high, low], axis=1), summer, preferred_element_type=F32
        )
        weight = jnp.exp(own + (sums[:, :rows] + carry))
        if diagonal:
            weight = jnp.where(causal, weight, 0.0)
        total = total + jnp.dot(weight.astype(BF16), v, preferred_element_type=F32)
        return carry + sums[:, rows:], total

    zero_carry = jnp.zeros((rows, rows), F32)
    zero_total = jnp.zeros((rows, HD), F32)

    for i in range(blocks):
        state = []
        for h in range(heads):
            state.extend(tile(i, i, h, zero_carry, zero_total, True))
        for j in range(i - 1, -1, -1):
            new = []
            for h in range(heads):
                new.extend(tile(i, j, h, state[2 * h], state[2 * h + 1], False))
            state = new
        out_ref[i] = jnp.concatenate([state[2 * h + 1] for h in range(heads)], axis=1).astype(BF16)


def attention(heads, qkv, shift):
    blocks, rows, _ = qkv.shape
    return pl.pallas_call(
        functools.partial(attention_kernel, heads),
        out_shape=jax.ShapeDtypeStruct((blocks, rows, heads * HD), BF16),
        in_specs=vmem(2),
        out_specs=vmem(1)[0],
        compiler_params=pltpu.CompilerParams(vmem_limit_bytes=VLIM),
        name="attention",
    )(qkv, shift)


def place(n_sp, n_dp):
    ny = n_sp // GROUPS
    sp, dp = lax.axis_index("sp"), lax.axis_index("dp")
    plane, y = sp // ny, lax.rem(sp, ny)
    member = y * n_dp + dp

    def at(g, m):
        return (g * ny + m // n_dp, lax.rem(m, n_dp))

    return plane, member, at


def partner(plane, d):
    if d == 1:
        return plane + 1 - 2 * lax.rem(plane, 2)
    if d == 2:
        return lax.rem(plane + 2, GROUPS)
    return 3 - plane if d == 3 else plane


def greet(plane, member, at, per_group):
    barrier = pltpu.get_barrier_semaphore()
    for d in range(1, GROUPS):
        pl.semaphore_signal(
            barrier, inc=1, device_id=at(lax.rem(plane + d, GROUPS), member), device_id_type=MESH
        )
    for d in range(1, per_group):
        pl.semaphore_signal(
            barrier, inc=1, device_id=at(plane, lax.rem(member + d, per_group)), device_id_type=MESH
        )
    pl.semaphore_wait(barrier, GROUPS + per_group - 2)


def one_hot_rows(meta, row):
    lanes = lax.broadcasted_iota(jnp.int32, (meta.shape[1], meta.shape[1]), 0).astype(F32)
    return lanes == meta[row : row + 1, :]


def dispatch_kernel(
    n_sp,
    n_dp,
    packed,
    meta,
    got,
    got_meta,
    block,
    stage,
    z_send,
    z_recv,
    t_send,
    t_recv,
    p_send,
    p_recv,
    own_sem,
):
    _, per_group, cap, width = got.shape
    slots = packed.shape[1]
    chunk = min(512, width)
    plane, member, at = place(n_sp, n_dp)
    greet(plane, member, at, per_group)
    z_copies, t_copies = {}, {}
    for d in (2, 3, 1):
        other = partner(plane, d)
        for kept, src, dst, send, recv in (
            (t_copies, meta, got_meta, t_send, t_recv),
            (z_copies, packed, block, z_send, z_recv),
        ):
            kept[d] = (
                pltpu.make_async_remote_copy(
                    src_ref=src.at[other],
                    dst_ref=dst.at[plane],
                    send_sem=send.at[d],
                    recv_sem=recv.at[d],
                    device_id=at(other, member),
                    device_id_type=MESH,
                )
            )
            kept[d].start()
    got_meta[plane] = meta[plane]
    later = []
    for d in (0, 2, 3, 1):
        source = partner(plane, d)
        if d:
            t_copies[d].wait_recv()
            z_copies[d].wait_recv()
        held = block if d else packed
        info = got_meta[source]
        hot = jnp.where(one_hot_rows(info, 0) | one_hot_rows(info, 1), 1.0, 0.0).astype(BF16)
        hot = hot[:, :slots]
        for c in range(0, width, chunk):
            rows = jnp.dot(hot, held[source, :, c : c + chunk], preferred_element_type=F32)
            for m in range(per_group):
                stage[source, m, :, c : c + chunk] = rows[m * cap : (m + 1) * cap].astype(BF16)
        own = pltpu.make_async_copy(stage.at[source, member], got.at[source, member], own_sem.at[d])
        own.start()
        later.append(own)
        for e in range(1, per_group):
            other = lax.rem(member + e, per_group)
            copy = pltpu.make_async_remote_copy(
                src_ref=stage.at[source, other],
                dst_ref=got.at[source, member],
                send_sem=p_send.at[d, e],
                recv_sem=p_recv.at[d, e],
                device_id=at(plane, other),
                device_id_type=MESH,
            )
            copy.start()
            later.append(copy)
    for copy in later:
        copy.wait()
    for d in range(1, GROUPS):
        t_copies[d].wait_send()
        z_copies[d].wait_send()


def dispatch(n_sp, n_dp, cap, packed, meta):
    per_group = n_sp * n_dp // GROUPS
    _, slots, width = packed.shape
    buffer = (GROUPS, per_group, cap, width)
    dma = pltpu.SemaphoreType.DMA
    return pl.pallas_call(
        functools.partial(dispatch_kernel, n_sp, n_dp),
        out_shape=[
            jax.ShapeDtypeStruct(buffer, BF16),
            jax.ShapeDtypeStruct(meta.shape, F32),
        ],
        in_specs=vmem(2),
        out_specs=vmem(2),
        scratch_shapes=[
            pltpu.VMEM(packed.shape, BF16),
            pltpu.VMEM(buffer, BF16),
            dma((GROUPS,)),
            dma((GROUPS,)),
            dma((GROUPS,)),
            dma((GROUPS,)),
            dma((GROUPS, per_group)),
            dma((GROUPS, per_group)),
            dma((GROUPS,)),
        ],
        compiler_params=pltpu.CompilerParams(
            collective_id=2, has_side_effects=True, vmem_limit_bytes=VLIM
        ),
        name="dispatch",
    )(packed, meta)


def combine_kernel(
    n_sp,
    n_dp,
    reply,
    meta,
    out,
    block,
    stage,
    z_send,
    z_recv,
    p_send,
    p_recv,
    own_sem,
):
    _, per_group, cap, width = reply.shape
    slots = out.shape[1]
    chunk = min(512, width)
    plane, member, at = place(n_sp, n_dp)
    greet(plane, member, at, per_group)
    order = (2, 3, 1, 0)
    plane_copies = {}
    for d in order:
        target = partner(plane, d)
        own = pltpu.make_async_copy(reply.at[target, member], block.at[target, member], own_sem.at[d])
        own.start()
        copies = [own]
        for e in range(1, per_group):
            other = lax.rem(member + e, per_group)
            copies.append(
                pltpu.make_async_remote_copy(
                    src_ref=reply.at[target, other],
                    dst_ref=block.at[target, member],
                    send_sem=p_send.at[d, e],
                    recv_sem=p_recv.at[d, e],
                    device_id=at(plane, other),
                    device_id_type=MESH,
                )
            )
            copies[-1].start()
        plane_copies[d] = copies
    z_copies = []
    for d in order:
        target = partner(plane, d)
        for copy in plane_copies[d]:
            copy.wait()
        info = meta[target]
        spread = jnp.where(one_hot_rows(info, 0), info[2:3, :], 0.0) + jnp.where(
            one_hot_rows(info, 1), info[3:4, :], 0.0
        )
        spread = spread.T[:slots]
        high = spread.astype(BF16)
        low = (spread - high.astype(F32)).astype(BF16)
        for c in range(0, width, chunk):
            if cap % 16 == 0:
                rows = block[target, :, :, c : c + chunk].reshape(per_group * cap, chunk)
            else:
                rows = jnp.concatenate(
                    [block[target, m, :, c : c + chunk].astype(F32) for m in range(per_group)], axis=0
                ).astype(BF16)
            total = jnp.dot(high, rows, preferred_element_type=F32) + jnp.dot(
                low, rows, preferred_element_type=F32
            )
            if d:
                stage[target, :, c : c + chunk] = total.astype(BF16)
            else:
                out[target, :, c : c + chunk] = total.astype(BF16)
        if d:
            copy = pltpu.make_async_remote_copy(
                src_ref=stage.at[target],
                dst_ref=out.at[plane],
                send_sem=z_send.at[d],
                recv_sem=z_recv.at[d],
                device_id=at(target, member),
                device_id_type=MESH,
            )
            copy.start()
            z_copies.append(copy)
    for copy in z_copies:
        copy.wait()


def combine(n_sp, n_dp, slots, reply, meta):
    _, per_group, cap, width = reply.shape
    dma = pltpu.SemaphoreType.DMA
    return pl.pallas_call(
        functools.partial(combine_kernel, n_sp, n_dp),
        out_shape=jax.ShapeDtypeStruct((GROUPS, slots, width), BF16),
        in_specs=vmem(2),
        out_specs=vmem(1)[0],
        scratch_shapes=[
            pltpu.VMEM(reply.shape, BF16),
            pltpu.VMEM((GROUPS, slots, width), BF16),
            dma((GROUPS,)),
            dma((GROUPS,)),
            dma((GROUPS, per_group)),
            dma((GROUPS, per_group)),
            dma((GROUPS,)),
        ],
        compiler_params=pltpu.CompilerParams(
            collective_id=3, has_side_effects=True, vmem_limit_bytes=VLIM
        ),
        name="combine",
    )(reply, meta)


def on_device(
    n_sp,
    n_dp,
    stream,
    queries,
    keys_in,
    values_in,
    key_shift,
    head_shift,
    mix_gain,
    out_weight,
    post_gain,
    route,
    route_weight,
    w_gate,
    w_up,
    w_down,
):
    tokens, width = stream.shape[1], stream.shape[2]
    heads = key_shift.shape[2] // n_sp
    cols = heads * HD

    n_expert = n_sp * n_dp
    per_group = n_expert // GROUPS
    cap = tokens // per_group
    slots = tokens // 2
    expert_ids = route[0].reshape(tokens * 2)
    onehot = (expert_ids[:, None] == jnp.arange(n_expert, dtype=jnp.int32)[None, :]).astype(BF16)
    before = jnp.arange(tokens * 2)
    earlier = (before[:, None] > before[None, :]).astype(BF16)
    counts = jnp.dot(earlier, onehot, preferred_element_type=F32)
    ranks = jnp.sum(counts * onehot.astype(F32), axis=1)
    inside = lax.rem(expert_ids, per_group).astype(F32) * cap + ranks
    inside = inside.reshape(tokens, 2)
    token_group = route[0][:, 0] // per_group
    group_hot = (token_group[:, None] == jnp.arange(GROUPS, dtype=jnp.int32)[None, :]).astype(BF16)
    group_rank = jnp.sum(
        jnp.dot(earlier[:tokens, :tokens], group_hot, preferred_element_type=F32)
        * group_hot.astype(F32),
        axis=1,
    )
    slot = token_group * slots + group_rank.astype(jnp.int32)
    slot_hot = slot[None, :] == jnp.arange(GROUPS * slots, dtype=jnp.int32)[:, None]
    facts = jnp.concatenate([inside + 1.0, route_weight[0]], axis=1)
    table = jnp.sum(jnp.where(slot_hot[:, None, :], facts.T[None, :, :], 0.0), axis=2)
    table = table - jnp.array([1.0, 1.0, 0.0, 0.0], F32)[None, :]
    table = table.reshape(GROUPS, slots, 4).transpose(0, 2, 1)
    lanes = per_group * cap
    meta = jnp.full((GROUPS, 8, lanes), -1.0, F32).at[:, :4, :slots].set(table)

    def by_peer(array):
        return array[0].reshape(tokens, n_sp, cols).transpose(1, 0, 2)

    qkv = jnp.concatenate([by_peer(queries), by_peer(keys_in), by_peer(values_in)], axis=2)
    offsets = (key_shift[0].astype(F32) + head_shift[None, :]).T.reshape(n_sp, heads, tokens)
    offsets = jnp.pad(offsets, ((0, 0), (0, 8 - heads), (0, 0)))
    qkv, offsets = swap(n_sp, 0, qkv, offsets)
    attended = attention(heads, qkv, offsets)
    (attended,) = swap(n_sp, 1, attended)
    att32 = attended.transpose(1, 0, 2).reshape(tokens, n_sp * cols).astype(F32)
    normed = (
        att32 * lax.rsqrt(jnp.mean(att32 * att32, axis=1, keepdims=True) + norm_eps) * mix_gain
    ).astype(BF16)
    mixed = jnp.dot(normed, out_weight, preferred_element_type=F32)
    summed = stream[0].astype(F32) + mixed
    hidden = (
        summed * lax.rsqrt(jnp.mean(summed * summed, axis=1, keepdims=True) + norm_eps) * post_gain
    ).astype(BF16)

    slot_hot = slot_hot.astype(BF16)
    packed = jnp.dot(slot_hot, hidden, preferred_element_type=F32).astype(BF16)
    received, tables = dispatch(n_sp, n_dp, cap, packed.reshape(GROUPS, slots, width), meta)
    rows = received.reshape(GROUPS * per_group * cap, width)
    gate = jnp.dot(rows, w_gate[0], preferred_element_type=F32)
    upper = jnp.dot(rows, w_up[0], preferred_element_type=F32)
    inner = (jax.nn.silu(gate) * upper).astype(BF16)
    reply = jnp.dot(inner, w_down[0], preferred_element_type=F32).astype(BF16)
    returned = combine(n_sp, n_dp, slots, reply.reshape(received.shape), tables)
    moe_sum = lax.dot_general(
        slot_hot,
        returned.reshape(GROUPS * slots, width),
        (((0,), (0,)), ((), ())),
        preferred_element_type=F32,
    )
    return (hidden.astype(F32) + moe_sum).astype(BF16)[None]


def solution(mesh):
    return jax.shard_map(
        functools.partial(on_device, mesh.shape["sp"], mesh.shape["dp"]),
        mesh=mesh,
        in_specs=(
            P("dp", "sp", None),
            P("dp", "sp", None),
            P("dp", "sp", None),
            P("dp", "sp", None),
            P("dp", "sp", None),
            P(),
            P(),
            P(),
            P(),
            P("dp", "sp", None),
            P("dp", "sp", None),
            P(("sp", "dp"), None, None),
            P(("sp", "dp"), None, None),
            P(("sp", "dp"), None, None),
        ),
        out_specs=P("dp", "sp", None),
        check_vma=False,
    )
```
